32 devices in a mesh: sp: 8 (over z, x), dp: 4 (over y, core).
Axes of the slice: x: 2, y: 2, z: 4, core: 2. Of those that a mesh axis runs over, the one named last changes fastest.
Arguments:
- queries: bfloat16 [4, 1024, 2048], P('dp', 'sp'), may hold values from -6 to 6
- keys: bfloat16 [4, 1024, 2048], P('dp', 'sp'), may hold values from -6 to 6
- values: bfloat16 [4, 1024, 2048], P('dp', 'sp'), may hold values from -6 to 6
- gate_totals: float32 [4, 1024, 32], P('dp', 'sp'), may hold values from -1024 to 0, as said below
- w_out: bfloat16 [2048, 2048], P(None, 'dp'), may hold values from -1 to 1
Outputs:
- mixed: bfloat16 [4, 1024, 2048], P('dp', 'sp')
The draws below stay inside these ranges and needn't reach their ends.
Inputs may be any that keep to these rules, and one draw needn't show every extreme that they name: `gate_totals`: never rising along a sequence.
All inputs are finite; a program needn't handle non-finite values.
Results may differ from the reference program's by a relative error of at most 0.0053.
Values may be sent and summed in bfloat16 or wider, within the bound.
A program may use at most 64 MiB of HBM per device.

```python
import math
import jax
import jax.numpy as jnp
from jax import lax

D = 2048
HEADS = 32
HEAD_DIM = 64
ATTN = 2048
LENGTH = 1024
BATCH = 4


def paired_draw(key):
    base = jax.random.fold_in(key, 11)
    first, second = jax.random.split(base, 2)
    shape = (BATCH, LENGTH, ATTN)
    query_draw = jnp.clip(jax.random.normal(first, shape, jnp.float32), -6.0, 6.0)
    key_draw = jnp.clip(jax.random.normal(second, shape, jnp.float32), -6.0, 6.0)
    return (query_draw, key_draw)


def draw_queries(key, part):
    return paired_draw(key)[0].astype(jnp.bfloat16)


def draw_keys(key, part):
    return paired_draw(key)[1].astype(jnp.bfloat16)


def draw_gate_totals(key, part):
    base = jax.random.fold_in(key, 23)
    first, second, third = jax.random.split(base, 3)
    fast_share = 0.5
    fast_heads = jax.random.bernoulli(first, fast_share, (BATCH, 1, HEADS))
    rates = jnp.where(fast_heads, 0.075, 1.2 / LENGTH).astype(jnp.float32)
    rough = jax.random.uniform(second, (BATCH, LENGTH, HEADS), jnp.float32, 0.3, 1.7)
    blocks = (LENGTH + 63) // 64
    block_scale = jnp.exp(jax.random.uniform(third, (BATCH, blocks, 1), jnp.float32, math.log(0.4), math.log(2.5)))
    block_scale = jnp.repeat(block_scale, 64, axis=1)[:, :LENGTH]
    log_gates = -rates * rough * block_scale
    return jnp.cumsum(log_gates, axis=1)


def level_of(stream_key, shape, cuts, least, top_value):
    level = 1.0
    for axis_at, parts in cuts:
        heights = jax.random.uniform(jax.random.fold_in(jax.random.fold_in(stream_key, 6), axis_at), (parts,), jnp.float32, least / len(cuts), top_value / len(cuts))
        level = level * jnp.repeat(jnp.exp(heights), shape[axis_at] // parts).reshape((-1,) + (1,) * (len(shape) - 1 - axis_at))
    return level


def bell_draw(stream_key, extent, width, bound, cuts=(), dtype=jnp.bfloat16):
    gain = level_of(stream_key, extent, cuts, -0.22, 0.18) if cuts else 1.0
    drawn = jax.random.normal(stream_key, extent, jnp.float32) * width * gain
    return jnp.minimum(jnp.maximum(drawn, -bound), bound).astype(dtype)


def setup_inputs(seed: int = 0) -> dict:
    splits = jax.random.split(jax.random.key(seed), 6)
    return {
        "queries": draw_queries(jax.random.fold_in(splits[5], 71), 0),
        "keys": draw_keys(jax.random.fold_in(splits[5], 71), 0),
        "values": bell_draw(splits[2], (BATCH, LENGTH, ATTN), 1.0, 6.0, ((0, 4), (1, 8))),
        "gate_totals": draw_gate_totals(jax.random.fold_in(splits[5], 71), 0),
        "w_out": bell_draw(splits[4], (ATTN, D), HEADS ** -0.5, 1.0, ((1, 4),)),
    }


def attend(queries, key_rows, value_rows, totals):
    length = queries.shape[0]
    block_rows = min(length, 512)
    pieces = []
    for begin_row in range(0, length, block_rows):
        end_row = begin_row + block_rows
        scores = jnp.einsum('qhd,khd->hqk', queries[begin_row:end_row].astype(jnp.float32), key_rows[:end_row].astype(jnp.float32)) * HEAD_DIM ** -0.5
        scores = scores + jnp.transpose(totals[begin_row:end_row])[:, :, None] - jnp.transpose(totals[:end_row])[:, None, :]
        causal = jnp.arange(end_row)[None, :] <= (begin_row + jnp.arange(block_rows))[:, None]
        scores = jnp.where(causal[None], scores, -jnp.inf)
        biggest = jnp.max(scores, axis=-1, keepdims=True)
        expo = jnp.exp(scores - biggest)
        summed = jnp.sum(expo, axis=-1)
        weights = expo.astype(jnp.bfloat16).astype(jnp.float32)
        output = jnp.einsum('hqk,khd->qhd', weights, value_rows[:end_row].astype(jnp.float32))
        output = output / jnp.transpose(summed)[:, :, None]
        pieces.append(output.astype(jnp.bfloat16))
    return jnp.concatenate(pieces, axis=0).reshape(length, -1)


def reference(queries, keys, values, gate_totals, w_out):
    shape4 = (BATCH, LENGTH, HEADS, HEAD_DIM)

    def one_sequence(items):
        return attend(items[0], items[1], items[2], items[3])

    attended = lax.map(one_sequence, (queries.reshape(shape4), keys.reshape(shape4), values.reshape(shape4), gate_totals))
    mixed = jnp.dot(attended.reshape(BATCH * LENGTH, ATTN), w_out, preferred_element_type=jnp.float32)
    return mixed.astype(jnp.bfloat16).reshape(BATCH, LENGTH, D)
```

```python
import functools

import jax
import jax.numpy as jnp
from jax import lax
from jax.experimental import pallas as pl
from jax.experimental.pallas import tpu as pltpu
from jax.sharding import PartitionSpec as P

HEAD_DIM = 64
LANES = 128
W_CHUNKS = 8
MESH = pl.DeviceIdType.MESH


def attend(queries, key_rows, value_rows, totals):
    length = queries.shape[0]
    block_rows = min(length, 512)
    pieces = []
    for begin_row in range(0, length, block_rows):
        end_row = begin_row + block_rows
        scaled = queries[begin_row:end_row] * jnp.bfloat16(HEAD_DIM ** (-0.5))
        scores = jnp.einsum(
            "qhd,khd->hqk", scaled, key_rows[:end_row], preferred_element_type=jnp.float32
        )
        causal = jnp.arange(end_row)[None, :] <= (begin_row + jnp.arange(block_rows))[:, None]
        scores = jnp.where(
            causal[None],
            scores
            + jnp.transpose(totals[begin_row:end_row])[:, :, None]
            - jnp.transpose(totals[:end_row])[:, None, :],
            -jnp.inf,
        )
        biggest = jnp.max(scores, axis=-1, keepdims=True)
        expo = jnp.exp(scores - biggest)
        summed = jnp.sum(expo, axis=-1)
        weights = expo.astype(jnp.bfloat16)
        output = jnp.einsum(
            "hqk,khd->qhd", weights, value_rows[:end_row], preferred_element_type=jnp.float32
        )
        output = output / jnp.transpose(summed)[:, :, None]
        pieces.append(output.astype(jnp.bfloat16))
    return jnp.concatenate(pieces, axis=0).reshape(length, -1)


def general(queries, keys, values, gate_totals, w_out):
    moved = [
        lax.all_to_all(x, "sp", split_axis=2, concat_axis=1, tiled=True)
        for x in (queries, keys, values, gate_totals)
    ]
    length = moved[0].shape[1]
    heads = [x[0].reshape(length, -1, HEAD_DIM) for x in moved[:3]]
    attended = attend(heads[0], heads[1], heads[2], moved[3][0])[None]
    rows = lax.all_to_all(attended, "sp", split_axis=1, concat_axis=2, tiled=True)
    mixed = jnp.dot(
        rows[0],
        lax.all_gather(w_out, "dp", axis=1, tiled=True),
        preferred_element_type=jnp.float32,
    )
    return mixed.astype(jnp.bfloat16)[None]


def kernel(n, ndp, q_ref, k_ref, v_ref, g_ref, w_ref, o_ref,
           qb, kb, vb, gb, ob, att, wall, acc,
           in_send, in_recv, g_send, g_recv, own_sem, o_send, o_recv,
           y_send, y_recv, p_send, p_recv, f_send, f_recv):
    me = lax.axis_index("sp")
    me_dp = lax.axis_index("dp")
    core = lax.rem(me_dp, 2)
    row_y = lax.div(me_dp, 2)
    ny = ndp // 2
    partner = row_y * 2 + 1 - core
    L = q_ref.shape[0]
    length = n * L
    pairs = qb.shape[0]
    W = pairs * LANES
    w_rows, w_cols = w_ref.shape
    step_rows = w_rows // W_CHUNKS

    barrier = pltpu.get_barrier_semaphore()
    for d in range(1, n):
        pl.semaphore_signal(barrier, inc=1, device_id={"sp": lax.rem(me + d, n)}, device_id_type=MESH)
    pl.semaphore_signal(barrier, inc=1, device_id={"dp": partner}, device_id_type=MESH)
    for d in range(1, ny):
        pl.semaphore_signal(
            barrier, inc=1, device_id={"dp": lax.rem(row_y + d, ny) * 2 + core}, device_id_type=MESH
        )
    pl.semaphore_wait(barrier, n - 1 + 1 + ny - 1)

    def rows_of(rank):
        return pl.ds(pl.multiple_of(rank * L, L), L)

    def lanes_of(rank, c):
        return pl.ds(pl.multiple_of(rank * W + c * LANES, LANES), LANES)

    bufs = ((k_ref, kb), (q_ref, qb), (v_ref, vb))

    def in_copy(a, c, d):
        dest = lax.rem(me + d, n)
        src, dst = bufs[a]
        return pltpu.make_async_remote_copy(
            src_ref=src.at[:, lanes_of(dest, c)], dst_ref=dst.at[c, rows_of(me), :],
            send_sem=in_send.at[a, c, d], recv_sem=in_recv.at[a, c, d],
            device_id={"sp": dest}, device_id_type=MESH)

    def in_own(a, c):
        src, dst = bufs[a]
        return pltpu.make_async_copy(src.at[:, lanes_of(me, c)], dst.at[c, rows_of(me), :], in_recv.at[a, c, 0])

    def g_copy(d):
        dest = lax.rem(me + d, n)
        return pltpu.make_async_remote_copy(
            src_ref=g_ref.at[dest], dst_ref=gb.at[me], send_sem=g_send.at[d], recv_sem=g_recv.at[d],
            device_id={"sp": dest}, device_id_type=MESH)

    def chunk(j):
        return pl.ds(j * step_rows, step_rows)

    def y_copy(d, j):
        return pltpu.make_async_remote_copy(
            src_ref=w_ref.at[chunk(j)], dst_ref=wall.at[me_dp, chunk(j)],
            send_sem=y_send.at[d, j], recv_sem=y_recv.at[d, j],
            device_id={"dp": lax.rem(row_y + d, ny) * 2 + core}, device_id_type=MESH)

    def source(d):
        return lax.rem(row_y + ny - d, ny) * 2

    def forward(d, j):
        held = source(d) + core
        return pltpu.make_async_remote_copy(
            src_ref=wall.at[held, chunk(j)], dst_ref=wall.at[held, chunk(j)],
            send_sem=f_send.at[d, j], recv_sem=f_recv.at[d, j],
            device_id={"dp": partner}, device_id_type=MESH)

    p_copy = pltpu.make_async_remote_copy(
        src_ref=w_ref, dst_ref=wall.at[me_dp], send_sem=p_send, recv_sem=p_recv,
        device_id={"dp": partner}, device_id_type=MESH)
    w_own = pltpu.make_async_copy(w_ref, wall.at[me_dp], own_sem.at[0])
    g_own = pltpu.make_async_copy(g_ref.at[me], gb.at[me], own_sem.at[1])

    for d in range(1, n):
        g_copy(d).start()
    for c in range(pairs):
        for d in range(1, n):
            for a in range(3):
                in_copy(a, c, d).start()
        if c == 0:
            for j in range(W_CHUNKS):
                for d in range(1, ny):
                    y_copy(d, j).start()
    g_own.start()
    for c in range(pairs):
        for a in range(3):
            in_own(a, c).start()
    p_copy.start()
    w_own.start()

    passed = [0]

    def pass_on(upto):
        for j in range(passed[0], min(upto, W_CHUNKS)):
            for d in range(1, ny):
                y_copy(d, j).wait_recv()
                forward(d, j).start()
        passed[0] = max(passed[0], min(upto, W_CHUNKS))

    def o_copy(c, d):
        dest = lax.rem(me + d, n)
        return pltpu.make_async_remote_copy(
            src_ref=ob.at[c, rows_of(dest), :], dst_ref=att.at[:, lanes_of(me, c)],
            send_sem=o_send.at[c, d], recv_sem=o_recv.at[c, d],
            device_id={"sp": dest}, device_id_type=MESH)

    def o_own(c):
        return pltpu.make_async_copy(ob.at[c, rows_of(me), :], att.at[:, lanes_of(me, c)], o_recv.at[c, 0])

    tile = 2 * L if n % 2 == 0 else L
    for c in range(pairs):
        if c == 0:
            g_own.wait()
            for d in range(1, n):
                g_copy(d).wait_recv()
        for a in range(3):
            in_own(a, c).wait()
        for d in range(1, n):
            for a in range(3):
                in_copy(a, c, d).wait_recv()
        for i in range(length // tile):
            kept = (i + 1) * tile
            rows = pl.ds(i * tile, tile)
            scaled = qb[c, rows, :] * jnp.bfloat16(HEAD_DIM ** -0.5)
            key_lane = lax.broadcasted_iota(jnp.int32, (kept, LANES), 1)
            out_lane = lax.broadcasted_iota(jnp.int32, (tile, LANES), 1)
            causal = lax.broadcasted_iota(jnp.int32, (tile, tile), 1) <= lax.broadcasted_iota(
                jnp.int32, (tile, tile), 0)
            keys = kb[c, pl.ds(0, kept), :]
            values = vb[c, pl.ds(0, kept), :]
            outs = []
            for h in range(2):
                mine = (key_lane < HEAD_DIM) if h == 0 else (key_lane >= HEAD_DIM)
                head_keys = jnp.where(mine, keys, jnp.zeros_like(keys))
                scores = lax.dot_general(
                    scaled, head_keys, (((1,), (1,)), ((), ())), preferred_element_type=jnp.float32)
                gates = jnp.concatenate(
                    [gb[b, 2 * c + h:2 * c + h + 1, :] for b in range(kept // L)], axis=1)
                scores = scores - gates
                last = jnp.where(causal, scores[:, kept - tile:], -jnp.inf)
                scores = last if i == 0 else jnp.concatenate([scores[:, :kept - tile], last], axis=1)
                peak = jnp.max(scores, axis=1, keepdims=True)
                expo = jnp.exp(scores - peak)
                total = jnp.sum(expo, axis=1, keepdims=True)
                outs.append(jnp.dot(
                    expo.astype(jnp.bfloat16), values, preferred_element_type=jnp.float32) / total)
            ob[c, rows, :] = jnp.where(out_lane < HEAD_DIM, outs[0], outs[1]).astype(jnp.bfloat16)
        for d in range(1, n):
            o_copy(c, d).start()
        o_own(c).start()
        pass_on((c + 1) * W_CHUNKS // (pairs + 2))

    for c in range(pairs):
        o_own(c).wait()
        for d in range(1, n):
            o_copy(c, d).wait_recv()

    def columns(r):
        return pl.ds(pl.multiple_of(r * w_cols, LANES), w_cols)

    w_own.wait()
    o_ref[:, columns(me_dp)] = jnp.dot(
        att[...], wall[me_dp], preferred_element_type=jnp.float32).astype(o_ref.dtype)
    p_copy.wait_recv()
    o_ref[:, columns(partner)] = jnp.dot(
        att[...], wall[partner], preferred_element_type=jnp.float32).astype(o_ref.dtype)
    for j in range(W_CHUNKS):
        pass_on(j + 1)
        for d in range(1, ny):
            straight = source(d) + core
            crossed = source(d) + 1 - core
            left = att[:, j * step_rows:(j + 1) * step_rows]
            for which, r in ((0, straight), (1, crossed)):
                if which:
                    forward(d, j).wait_recv()
                part = jnp.dot(left, wall[r, chunk(j)], preferred_element_type=jnp.float32)
                if j > 0:
                    part = acc[d - 1, which] + part
                if j < W_CHUNKS - 1:
                    acc[d - 1, which] = part
                else:
                    o_ref[:, columns(r)] = part.astype(o_ref.dtype)

    p_copy.wait_send()
    for d in range(1, n):
        g_copy(d).wait_send()
        for c in range(pairs):
            o_copy(c, d).wait_send()
            for a in range(3):
                in_copy(a, c, d).wait_send()
    for j in range(W_CHUNKS):
        for d in range(1, ny):
            y_copy(d, j).wait_send()
            forward(d, j).wait_send()


def fused(n, ndp, queries, keys, values, gate_totals, w_out):
    L, model = queries.shape[1], queries.shape[2]
    heads = gate_totals.shape[2] // n
    pairs = heads * HEAD_DIM // LANES
    length = n * L
    ny = ndp // 2
    gates = jnp.transpose(gate_totals[0]).reshape(n, heads, L)
    w_rows, w_cols = w_out.shape
    bf16, f32 = jnp.bfloat16, jnp.float32
    dma = pltpu.SemaphoreType.DMA
    anywhere = pl.BlockSpec(memory_space=pl.ANY)
    out = pl.pallas_call(
        functools.partial(kernel, n, ndp),
        out_shape=jax.ShapeDtypeStruct((L, w_cols * ndp), bf16),
        in_specs=[anywhere] * 5,
        out_specs=pl.BlockSpec(memory_space=pltpu.VMEM),
        scratch_shapes=[
            pltpu.VMEM((pairs, length, LANES), bf16),
            pltpu.VMEM((pairs, length, LANES), bf16),
            pltpu.VMEM((pairs, length, LANES), bf16),
            pltpu.VMEM((n, heads, L), f32),
            pltpu.VMEM((pairs, length, LANES), bf16),
            pltpu.VMEM((L, model), bf16),
            pltpu.VMEM((ndp, w_rows, w_cols), bf16),
            pltpu.VMEM((max(ny - 1, 1), 2, L, w_cols), f32),
            dma((3, pairs, n)), dma((3, pairs, n)), dma((n,)), dma((n,)), dma((2,)),
            dma((pairs, n)), dma((pairs, n)),
            dma((ny, W_CHUNKS)), dma((ny, W_CHUNKS)), dma, dma,
            dma((ny, W_CHUNKS)), dma((ny, W_CHUNKS)),
        ],
        compiler_params=pltpu.CompilerParams(
            collective_id=0, has_side_effects=True, vmem_limit_bytes=48 * 1024 * 1024),
        name="fused_attention",
    )(queries[0], keys[0], values[0], gates, w_out)
    return out[None]


def solution(mesh):
    n, ndp = mesh.shape["sp"], mesh.shape["dp"]

    def local(queries, keys, values, gate_totals, w_out):
        width = queries.shape[2] // n
        fits = width % LANES == 0 and ndp % 2 == 0 and queries.shape[1] % LANES == 0
        if fits:
            return fused(n, ndp, queries, keys, values, gate_totals, w_out)
        return general(queries, keys, values, gate_totals, w_out)

    placed = (P("dp", "sp", None),) * 4 + (P(None, "dp"),)
    return jax.shard_map(
        local, mesh=mesh, in_specs=placed, out_specs=P("dp", "sp", None), check_vma=False)
```

```python
import functools

import jax
import jax.numpy as jnp
from jax import lax
from jax.experimental import pallas as pl
from jax.experimental.pallas import tpu as pltpu
from jax.sharding import PartitionSpec as P

HEAD_DIM = 64
LANES = 128
W_CHUNKS = 8
MESH = pl.DeviceIdType.MESH


def attend(queries, key_rows, value_rows, totals):
    length = queries.shape[0]
    block_rows = min(length, 512)
    pieces = []
    for begin_row in range(0, length, block_rows):
        end_row = begin_row + block_rows
        scaled = queries[begin_row:end_row] * jnp.bfloat16(HEAD_DIM ** (-0.5))
        scores = jnp.einsum(
            "qhd,khd->hqk", scaled, key_rows[:end_row], preferred_element_type=jnp.float32
        )
        causal = jnp.arange(end_row)[None, :] <= (begin_row + jnp.arange(block_rows))[:, None]
        scores = jnp.where(
            causal[None],
            scores
            + jnp.transpose(totals[begin_row:end_row])[:, :, None]
            - jnp.transpose(totals[:end_row])[:, None, :],
            -jnp.inf,
        )
        biggest = jnp.max(scores, axis=-1, keepdims=True)
        expo = jnp.exp(scores - biggest)
        summed = jnp.sum(expo, axis=-1)
        weights = expo.astype(jnp.bfloat16)
        output = jnp.einsum(
            "hqk,khd->qhd", weights, value_rows[:end_row], preferred_element_type=jnp.float32
        )
        output = output / jnp.transpose(summed)[:, :, None]
        pieces.append(output.astype(jnp.bfloat16))
    return jnp.concatenate(pieces, axis=0).reshape(length, -1)


def general(queries, keys, values, gate_totals, w_out):
    moved = [
        lax.all_to_all(x, "sp", split_axis=2, concat_axis=1, tiled=True)
        for x in (queries, keys, values, gate_totals)
    ]
    length = moved[0].shape[1]
    heads = [x[0].reshape(length, -1, HEAD_DIM) for x in moved[:3]]
    attended = attend(heads[0], heads[1], heads[2], moved[3][0])[None]
    rows = lax.all_to_all(attended, "sp", split_axis=1, concat_axis=2, tiled=True)
    mixed = jnp.dot(
        rows[0],
        lax.all_gather(w_out, "dp", axis=1, tiled=True),
        preferred_element_type=jnp.float32,
    )
    return mixed.astype(jnp.bfloat16)[None]


def attend_rows(queries, parts, diagonal):
    rows = queries.shape[0]
    scaled = queries * jnp.bfloat16(HEAD_DIM ** -0.5)
    lane = lax.broadcasted_iota(jnp.int32, (rows, LANES), 1)
    outs, sums = [], []
    for h in range(2):
        mine = (lane < HEAD_DIM) if h == 0 else (lane >= HEAD_DIM)
        scores = []
        for at, (keys, _, gates) in enumerate(parts):
            head_keys = jnp.where(mine, keys, jnp.zeros_like(keys))
            score = lax.dot_general(
                scaled, head_keys, (((1,), (1,)), ((), ())), preferred_element_type=jnp.float32)
            score = score - gates[h:h + 1, :]
            if diagonal and at == len(parts) - 1:
                causal = lax.broadcasted_iota(jnp.int32, score.shape, 1) <= lax.broadcasted_iota(
                    jnp.int32, score.shape, 0)
                score = jnp.where(causal, score, -jnp.inf)
            scores.append(score)
        peak = functools.reduce(jnp.maximum, [jnp.max(x, axis=1, keepdims=True) for x in scores])
        expo = [jnp.exp(x - peak) for x in scores]
        total = sum(jnp.sum(x, axis=1, keepdims=True) for x in expo)
        out = sum(
            jnp.dot(x.astype(jnp.bfloat16), part[1], preferred_element_type=jnp.float32)
            for x, part in zip(expo, parts))
        outs.append(out / total)
        sums.append(peak + jnp.log(total))
    first = lane < HEAD_DIM
    return jnp.where(first, outs[0], outs[1]), jnp.where(first, sums[0], sums[1])


def kernel(n, ndp, q_ref, k_ref, v_ref, g_ref, w_ref, o_ref,
           qx, kx, vx, kz, vz, qz, gb, ob, held_o, held_l, part_o, part_l, got_o, got_l, att, wall, acc,
           x_send, x_recv, g_send, g_recv, own_sem, z_send, z_recv, po_send, po_recv, pl_send, pl_recv,
           o_send, o_recv, y_send, y_recv, wx_send, wx_recv, p_send, p_recv, f_send, f_recv):
    me = lax.axis_index("sp")
    x = lax.rem(me, 2)
    z = lax.div(me, 2)
    side = me + 1 - 2 * x
    me_dp = lax.axis_index("dp")
    core = lax.rem(me_dp, 2)
    row_y = lax.div(me_dp, 2)
    across = (1 - row_y) * 2 + core
    partner = row_y * 2 + 1 - core
    L = q_ref.shape[0]
    pairs = qx.shape[0]
    W = pairs * LANES
    w_rows, w_cols = w_ref.shape
    step_rows = w_rows // W_CHUNKS
    lent = W_CHUNKS // 4
    direct = W_CHUNKS - lent

    barrier = pltpu.get_barrier_semaphore()
    for d in range(1, n):
        pl.semaphore_signal(barrier, inc=1, device_id={"sp": lax.rem(me + d, n)}, device_id_type=MESH)
    for other in (partner, across):
        pl.semaphore_signal(barrier, inc=1, device_id={"dp": other}, device_id_type=MESH)
    pl.semaphore_wait(barrier, n + 1)

    def remote(src, dst, send, recv, **device):
        return pltpu.make_async_remote_copy(
            src_ref=src, dst_ref=dst, send_sem=send, recv_sem=recv, device_id=device, device_id_type=MESH)

    def rows_of(which):
        return pl.ds(pl.multiple_of(which * L, L), L)

    def lanes_of(which, p):
        return pl.ds(pl.multiple_of(which * W + p * LANES, LANES), LANES)

    bufs = ((q_ref, qx), (k_ref, kx), (v_ref, vx))

    def x_copy(a, p):
        src, dst = bufs[a]
        return remote(src.at[:, lanes_of(1 - x, p)], dst.at[p, rows_of(x), :],
                      x_send.at[a, p], x_recv.at[a, p], sp=side)

    def x_own(a, p):
        src, dst = bufs[a]
        return pltpu.make_async_copy(src.at[:, lanes_of(x, p)], dst.at[p, rows_of(x), :], own_sem.at[a, p])

    def g_copy(d):
        dest = lax.rem(me + d, n)
        return remote(g_ref.at[lax.rem(dest, 2)], gb.at[me], g_send.at[d], g_recv.at[d], sp=dest)

    g_own = pltpu.make_async_copy(g_ref.at[x], gb.at[me], g_recv.at[0])

    def chunk(s):
        if s < lent:
            at = s + direct * x
        elif s < direct:
            at = s
        else:
            at = (s - direct) + direct * (1 - x)
        return pl.ds(pl.multiple_of(at * step_rows, step_rows), step_rows)

    def y_copy(s):
        return remote(w_ref.at[chunk(s)], wall.at[me_dp, chunk(s)], y_send.at[s], y_recv.at[s], dp=across)

    def lend(s):
        return remote(wall.at[across, chunk(s)], wall.at[across, chunk(s)], wx_send.at[s], wx_recv.at[s], sp=side)

    def forward(s):
        return remote(wall.at[across, chunk(s)], wall.at[across, chunk(s)], f_send.at[s], f_recv.at[s], dp=partner)

    p_copy = remote(w_ref, wall.at[me_dp], p_send, p_recv, dp=partner)
    w_own = pltpu.make_async_copy(w_ref, wall.at[me_dp], own_sem.at[3, 0])

    for p in range(pairs):
        for a in range(3):
            x_copy(a, p).start()
        if p == 0:
            for d in range(1, n):
                g_copy(d).start()
            for s in range(direct):
                y_copy(s).start()
            g_own.start()
        for a in range(3):
            x_own(a, p).start()
    p_copy.start()
    w_own.start()

    def pass_on(begin, end):
        for s in range(begin, end):
            if s < direct:
                y_copy(s).wait_recv()
            else:
                lend(s - direct).wait_recv()
            forward(s).start()
            if s < lent:
                lend(s).start()

    def arrived(p):
        for a in range(3):
            x_own(a, p).wait()
            x_copy(a, p).wait_recv()

    def to_z(src, dst, k, slot, p, target):
        return remote(src, dst, z_send.at[k, p], z_recv.at[slot, p], sp=target * 2 + x)

    def part_copies(k, slot, p, target):
        return (
            remote(part_o.at[k, p], got_o.at[slot, p], po_send.at[k, p], po_recv.at[slot, p], sp=target * 2 + x),
            remote(part_l.at[k, p], got_l.at[slot, p], pl_send.at[k, p], pl_recv.at[slot, p], sp=target * 2 + x),
        )

    def o_copy(p):
        return remote(ob.at[p, rows_of(1 - x), :], att.at[:, lanes_of(x, p)], o_send.at[p], o_recv.at[p], sp=side)

    def o_own(p):
        return pltpu.make_async_copy(ob.at[p, rows_of(x), :], att.at[:, lanes_of(x, p)], own_sem.at[3, 1 + p])

    def gates_of(block, p):
        return jnp.concatenate([gb[2 * block, p], gb[2 * block + 1, p]], axis=1)

    def finish(p, value):
        ob[p] = value.astype(jnp.bfloat16)
        o_copy(p).start()
        o_own(p).start()

    def share(p, k, slot, target, value, lse):
        part_o[k, p] = value.astype(jnp.bfloat16)
        turned = jnp.transpose(lse)
        part_l[k, p] = jnp.concatenate([turned[0:1], turned[HEAD_DIM:HEAD_DIM + 1]], axis=0)
        for copy in part_copies(k, slot, p, target):
            copy.start()

    def join(p, slots):
        outs, sums = [held_o[p]], [held_l[p]]
        for slot in slots:
            for copy in part_copies(0, slot, p, 0):
                copy.wait_recv()
            outs.append(got_o[slot, p].astype(jnp.float32))
            lse = got_l[slot, p]
            sums.append(jnp.transpose(jnp.concatenate(
                [jnp.broadcast_to(lse[h:h + 1], (HEAD_DIM, 2 * L)) for h in range(2)], axis=0)))
        peak = functools.reduce(jnp.maximum, sums)
        scale = [jnp.exp(s - peak) for s in sums]
        finish(p, sum(o * s for o, s in zip(outs, scale)) / sum(scale))

    def each(body, begin=0, end=None):
        def step(p, carry):
            body(p)
            return carry
        lax.fori_loop(begin, pairs if end is None else end, step, 0)

    def gates_here():
        g_own.wait()
        for d in range(1, n):
            g_copy(d).wait_recv()

    half = pairs // 2

    @pl.when(z == 0)
    def _():
        def push(p):
            arrived(p)
            to_z(kx.at[p], kz.at[p], 0, 0, p, 1).start()
            to_z(vx.at[p], vz.at[p], 1, 1, p, 1).start()
        each(push)
        gates_here()
        def work(p):
            finish(p, attend_rows(qx[p], [(kx[p], vx[p], gates_of(0, p))], True)[0])
        each(work)
        pass_on(0, lent)
        def left(p):
            to_z(kx.at[p], kz.at[p], 0, 0, p, 1).wait_send()
            to_z(vx.at[p], vz.at[p], 1, 1, p, 1).wait_send()
        each(left)

    @pl.when(z == 1)
    def _():
        gates_here()
        def work(p):
            arrived(p)
            to_z(kx.at[p], kz.at[p], 0, 0, p, 0).wait_recv()
            to_z(vx.at[p], vz.at[p], 1, 1, p, 0).wait_recv()
            lower = (kz[p], vz[p], gates_of(0, p))
            own = (kx[p], vx[p], gates_of(1, p))
            finish(p, attend_rows(qx[p], [lower, own], True)[0])
            for k in range(2):
                to_z(qx.at[p], qz.at[k, p], 0, 2 + k, p, 0).wait_recv()
                share(p, k, 0, 2 + k, *attend_rows(qz[k, p], [lower, own], False))
        each(work, 0, half)
        pass_on(0, lent)
        each(work, half)
        def left(p):
            for k in range(2):
                for copy in part_copies(k, 0, p, 2 + k):
                    copy.wait_send()
        each(left)

    @pl.when(z == 2)
    def _():
        def push(p):
            arrived(p)
            to_z(qx.at[p], qz.at[0, p], 0, 2, p, 1).start()
        each(push)
        gates_here()
        def work(p):
            own = (kx[p], vx[p], gates_of(2, p))
            held_o[p], held_l[p] = attend_rows(qx[p], [own], True)
            to_z(qx.at[p], qz.at[0, p], 0, 2, p, 1).wait_recv()
            share(p, 1, 1, 3, *attend_rows(qz[0, p], [own], False))
        each(work)
        pass_on(0, lent)
        each(lambda p: join(p, (0,)))
        def left(p):
            to_z(qx.at[p], qz.at[0, p], 0, 2, p, 1).wait_send()
            for copy in part_copies(1, 1, p, 3):
                copy.wait_send()
        each(left)

    @pl.when(z == 3)
    def _():
        def push(p):
            arrived(p)
            to_z(qx.at[p], qz.at[1, p], 0, 3, p, 1).start()
            to_z(qx.at[p], qz.at[0, p], 1, 2, p, 2).start()
        each(push)
        gates_here()
        def work(p):
            held_o[p], held_l[p] = attend_rows(qx[p], [(kx[p], vx[p], gates_of(3, p))], True)
        each(work)
        pass_on(0, lent)
        each(lambda p: join(p, (0, 1)))
        def left(p):
            to_z(qx.at[p], qz.at[1, p], 0, 3, p, 1).wait_send()
            to_z(qx.at[p], qz.at[0, p], 1, 2, p, 2).wait_send()
        each(left)

    def whole(p):
        o_own(p).wait()
        o_copy(p).wait_recv()
    each(whole)

    def columns(r):
        return pl.ds(pl.multiple_of(r * w_cols, LANES), w_cols)

    pass_on(lent, W_CHUNKS // 2)
    w_own.wait()
    o_ref[:, columns(me_dp)] = jnp.dot(
        att[...], wall[me_dp], preferred_element_type=jnp.float32).astype(o_ref.dtype)
    p_copy.wait_recv()
    o_ref[:, columns(partner)] = jnp.dot(
        att[...], wall[partner], preferred_element_type=jnp.float32).astype(o_ref.dtype)
    crossed = (1 - row_y) * 2 + 1 - core
    order = list(range(lent)) + list(range(direct, W_CHUNKS)) + list(range(lent, direct))
    for at, s in enumerate(order):
        if s >= W_CHUNKS // 2:
            pass_on(s, s + 1)
        left = att[:, chunk(s)]
        for which, r in ((0, across), (1, crossed)):
            if which:
                forward(s).wait_recv()
            part = jnp.dot(left, wall[r, chunk(s)], preferred_element_type=jnp.float32)
            if at > 0:
                part = acc[which] + part
            if at < W_CHUNKS - 1:
                acc[which] = part
            else:
                o_ref[:, columns(r)] = part.astype(o_ref.dtype)

    p_copy.wait_send()
    for d in range(1, n):
        g_copy(d).wait_send()
    def sent(p):
        o_copy(p).wait_send()
        for a in range(3):
            x_copy(a, p).wait_send()
    each(sent)
    for s in range(W_CHUNKS):
        if s < direct:
            y_copy(s).wait_send()
        if s < lent:
            lend(s).wait_send()
        forward(s).wait_send()


def fused(n, ndp, queries, keys, values, gate_totals, w_out):
    L, model = queries.shape[1], queries.shape[2]
    heads = gate_totals.shape[2] // 2
    pairs = heads * HEAD_DIM // LANES
    gates = jnp.transpose(gate_totals[0]).reshape(2, pairs, 2, L)
    w_rows, w_cols = w_out.shape
    bf16, f32 = jnp.bfloat16, jnp.float32
    dma = pltpu.SemaphoreType.DMA
    block = (pairs, 2 * L, LANES)
    out = pl.pallas_call(
        functools.partial(kernel, n, ndp),
        out_shape=jax.ShapeDtypeStruct((L, w_cols * ndp), bf16),
        in_specs=[pl.BlockSpec(memory_space=pl.ANY)] * 5,
        out_specs=pl.BlockSpec(memory_space=pltpu.VMEM),
        scratch_shapes=[
            *[pltpu.VMEM(block, bf16)] * 5,
            pltpu.VMEM((2,) + block, bf16),
            pltpu.VMEM((n, pairs, 2, L), f32),
            pltpu.VMEM(block, bf16),
            pltpu.VMEM(block, f32),
            pltpu.VMEM(block, f32),
            pltpu.VMEM((2,) + block, bf16),
            pltpu.VMEM((2, pairs, 2, 2 * L), f32),
            pltpu.VMEM((2,) + block, bf16),
            pltpu.VMEM((2, pairs, 2, 2 * L), f32),
            pltpu.VMEM((L, model), bf16),
            pltpu.VMEM((ndp, w_rows, w_cols), bf16),
            pltpu.VMEM((2, L, w_cols), f32),
            dma((3, pairs)), dma((3, pairs)), dma((n,)), dma((n,)), dma((4, pairs + 1)),
            dma((2, pairs)), dma((4, pairs)),
            dma((2, pairs)), dma((2, pairs)), dma((2, pairs)), dma((2, pairs)),
            dma((pairs,)), dma((pairs,)),
            dma((W_CHUNKS,)), dma((W_CHUNKS,)), dma((W_CHUNKS,)), dma((W_CHUNKS,)), dma, dma,
            dma((W_CHUNKS,)), dma((W_CHUNKS,)),
        ],
        compiler_params=pltpu.CompilerParams(
            collective_id=0, has_side_effects=True, vmem_limit_bytes=67043328),
        name="fused_attention",
    )(queries[0], keys[0], values[0], gates, w_out)
    return out[None]


def solution(mesh):
    n, ndp = mesh.shape["sp"], mesh.shape["dp"]

    def local(queries, keys, values, gate_totals, w_out):
        fits = n == 8 and ndp == 4 and queries.shape[1] % LANES == 0
        if fits:
            return fused(n, ndp, queries, keys, values, gate_totals, w_out)
        return general(queries, keys, values, gate_totals, w_out)

    placed = (P("dp", "sp", None),) * 4 + (P(None, "dp"),)
    return jax.shard_map(
        local, mesh=mesh, in_specs=placed, out_specs=P("dp", "sp", None), check_vma=False)
```

```python
import functools

import jax
import jax.numpy as jnp
from jax import lax
from jax.experimental import pallas as pl
from jax.experimental.pallas import tpu as pltpu
from jax.sharding import PartitionSpec as P

HEAD_DIM = 64
LANES = 128
W_CHUNKS = 8
MESH = pl.DeviceIdType.MESH


def attend(queries, key_rows, value_rows, totals):
    length = queries.shape[0]
    block_rows = min(length, 512)
    pieces = []
    for begin_row in range(0, length, block_rows):
        end_row = begin_row + block_rows
        scaled = queries[begin_row:end_row] * jnp.bfloat16(HEAD_DIM ** (-0.5))
        scores = jnp.einsum(
            "qhd,khd->hqk", scaled, key_rows[:end_row], preferred_element_type=jnp.float32
        )
        causal = jnp.arange(end_row)[None, :] <= (begin_row + jnp.arange(block_rows))[:, None]
        scores = jnp.where(
            causal[None],
            scores
            + jnp.transpose(totals[begin_row:end_row])[:, :, None]
            - jnp.transpose(totals[:end_row])[:, None, :],
            -jnp.inf,
        )
        biggest = jnp.max(scores, axis=-1, keepdims=True)
        expo = jnp.exp(scores - biggest)
        summed = jnp.sum(expo, axis=-1)
        weights = expo.astype(jnp.bfloat16)
        output = jnp.einsum(
            "hqk,khd->qhd", weights, value_rows[:end_row], preferred_element_type=jnp.float32
        )
        output = output / jnp.transpose(summed)[:, :, None]
        pieces.append(output.astype(jnp.bfloat16))
    return jnp.concatenate(pieces, axis=0).reshape(length, -1)


def general(queries, keys, values, gate_totals, w_out):
    moved = [
        lax.all_to_all(x, "sp", split_axis=2, concat_axis=1, tiled=True)
        for x in (queries, keys, values, gate_totals)
    ]
    length = moved[0].shape[1]
    heads = [x[0].reshape(length, -1, HEAD_DIM) for x in moved[:3]]
    attended = attend(heads[0], heads[1], heads[2], moved[3][0])[None]
    rows = lax.all_to_all(attended, "sp", split_axis=1, concat_axis=2, tiled=True)
    mixed = jnp.dot(
        rows[0],
        lax.all_gather(w_out, "dp", axis=1, tiled=True),
        preferred_element_type=jnp.float32,
    )
    return mixed.astype(jnp.bfloat16)[None]


def attend_rows(queries, parts, diagonal):
    rows = queries.shape[0]
    scaled = queries * jnp.bfloat16(HEAD_DIM ** -0.5)
    lane = lax.broadcasted_iota(jnp.int32, (rows, LANES), 1)
    outs, sums = [], []
    for h in range(2):
        mine = (lane < HEAD_DIM) if h == 0 else (lane >= HEAD_DIM)
        scores = []
        for at, (keys, _, gates) in enumerate(parts):
            head_keys = jnp.where(mine, keys, jnp.zeros_like(keys))
            score = lax.dot_general(
                scaled, head_keys, (((1,), (1,)), ((), ())), preferred_element_type=jnp.float32)
            score = score - gates[h:h + 1, :]
            if diagonal and at == len(parts) - 1:
                causal = lax.broadcasted_iota(jnp.int32, score.shape, 1) <= lax.broadcasted_iota(
                    jnp.int32, score.shape, 0)
                score = jnp.where(causal, score, -jnp.inf)
            scores.append(score)
        peak = functools.reduce(jnp.maximum, [jnp.max(x, axis=1, keepdims=True) for x in scores])
        expo = [jnp.exp(x - peak) for x in scores]
        total = sum(jnp.sum(x, axis=1, keepdims=True) for x in expo)
        out = sum(
            jnp.dot(x.astype(jnp.bfloat16), part[1], preferred_element_type=jnp.float32)
            for x, part in zip(expo, parts))
        outs.append(out / total)
        sums.append(peak + jnp.log(total))
    first = lane < HEAD_DIM
    return jnp.where(first, outs[0], outs[1]), jnp.where(first, sums[0], sums[1])


def kernel(n, ndp, q_ref, k_ref, v_ref, g_ref, w_ref, o_ref,
           qx, kx, vx, kz, vz, qz, gb, ob, held_o, held_l, part_o, part_l, got_o, got_l, att, wall, acc,
           x_send, x_recv, g_send, g_recv, own_sem, z_send, z_recv, po_send, po_recv, pl_send, pl_recv,
           o_send, o_recv, y_send, y_recv, wx_send, wx_recv, p_send, p_recv, f_send, f_recv):
    me = lax.axis_index("sp")
    x = lax.rem(me, 2)
    z = lax.div(me, 2)
    side = me + 1 - 2 * x
    me_dp = lax.axis_index("dp")
    core = lax.rem(me_dp, 2)
    row_y = lax.div(me_dp, 2)
    across = (1 - row_y) * 2 + core
    partner = row_y * 2 + 1 - core
    L = q_ref.shape[0]
    pairs = qx.shape[0]
    W = pairs * LANES
    w_rows, w_cols = w_ref.shape
    step_rows = w_rows // W_CHUNKS
    lent = W_CHUNKS // 4
    direct = W_CHUNKS - lent

    barrier = pltpu.get_barrier_semaphore()
    meets = {0: (1,), 1: (0, 2, 3), 2: (1, 3), 3: (1, 2)}
    for here, others in meets.items():
        @pl.when(z == here)
        def _(others=others):
            for other in others:
                pl.semaphore_signal(barrier, inc=1, device_id={"sp": other * 2 + x}, device_id_type=MESH)
    pl.semaphore_signal(barrier, inc=1, device_id={"sp": side}, device_id_type=MESH)
    for other in (partner, across):
        pl.semaphore_signal(barrier, inc=1, device_id={"dp": other}, device_id_type=MESH)
    for here, others in meets.items():
        @pl.when(z == here)
        def _(others=others):
            pl.semaphore_wait(barrier, len(others) + 3)

    def remote(src, dst, send, recv, **device):
        return pltpu.make_async_remote_copy(
            src_ref=src, dst_ref=dst, send_sem=send, recv_sem=recv, device_id=device, device_id_type=MESH)

    def rows_of(which):
        return pl.ds(pl.multiple_of(which * L, L), L)

    def lanes_of(which, p):
        return pl.ds(pl.multiple_of(which * W + p * LANES, LANES), LANES)

    bufs = ((q_ref, qx), (k_ref, kx), (v_ref, vx))

    def x_copy(a, p):
        src, dst = bufs[a]
        return remote(src.at[:, lanes_of(1 - x, p)], dst.at[p, rows_of(x), :],
                      x_send.at[a, p], x_recv.at[a, p], sp=side)

    def x_own(a, p):
        src, dst = bufs[a]
        return pltpu.make_async_copy(src.at[:, lanes_of(x, p)], dst.at[p, rows_of(x), :], own_sem.at[a, p])

    g_copy = remote(g_ref.at[1 - x], gb.at[me], g_send.at[0], g_recv.at[0], sp=side)
    g_own = pltpu.make_async_copy(g_ref.at[x], gb.at[me], g_recv.at[1])

    def chunk(s):
        if s < lent:
            at = s + direct * x
        elif s < direct:
            at = s
        else:
            at = (s - direct) + direct * (1 - x)
        return pl.ds(pl.multiple_of(at * step_rows, step_rows), step_rows)

    def y_copy(s):
        return remote(w_ref.at[chunk(s)], wall.at[me_dp, chunk(s)], y_send.at[s], y_recv.at[s], dp=across)

    def lend(s):
        return remote(wall.at[across, chunk(s)], wall.at[across, chunk(s)], wx_send.at[s], wx_recv.at[s], sp=side)

    def forward(s):
        return remote(wall.at[across, chunk(s)], wall.at[across, chunk(s)], f_send.at[s], f_recv.at[s], dp=partner)

    p_copy = remote(w_ref, wall.at[me_dp], p_send, p_recv, dp=partner)
    w_own = pltpu.make_async_copy(w_ref, wall.at[me_dp], own_sem.at[3, 0])

    for p in range(pairs):
        for a in range(3):
            x_copy(a, p).start()
        if p == 0:
            g_copy.start()
            for s in range(direct):
                y_copy(s).start()
            g_own.start()
        for a in range(3):
            x_own(a, p).start()
    p_copy.start()
    w_own.start()

    def pass_on(begin, end):
        for s in range(begin, end):
            if s < direct:
                y_copy(s).wait_recv()
            else:
                lend(s - direct).wait_recv()
            forward(s).start()
            if s < lent:
                lend(s).start()

    def arrived(p):
        for a in range(3):
            x_own(a, p).wait()
            x_copy(a, p).wait_recv()

    def to_z(src, dst, k, slot, p, target):
        return remote(src, dst, z_send.at[k, p], z_recv.at[slot, p], sp=target * 2 + x)

    def part_copies(k, slot, p, target):
        return (
            remote(part_o.at[k, p], got_o.at[slot, p], po_send.at[k, p], po_recv.at[slot, p], sp=target * 2 + x),
            remote(part_l.at[k, p], got_l.at[slot, p], pl_send.at[k, p], pl_recv.at[slot, p], sp=target * 2 + x),
        )

    def o_copy(p):
        return remote(ob.at[p, rows_of(1 - x), :], att.at[:, lanes_of(x, p)], o_send.at[p], o_recv.at[p], sp=side)

    def o_own(p):
        return pltpu.make_async_copy(ob.at[p, rows_of(x), :], att.at[:, lanes_of(x, p)], own_sem.at[3, 1 + p])

    def gates_of(block, p):
        return jnp.concatenate([gb[2 * block, p], gb[2 * block + 1, p]], axis=1)

    def finish(p, value):
        ob[p] = value.astype(jnp.bfloat16)
        o_copy(p).start()
        o_own(p).start()

    def share(p, k, slot, target, value, lse):
        part_o[k, p] = value.astype(jnp.bfloat16)
        turned = jnp.transpose(lse)
        part_l[k, p] = jnp.concatenate([turned[0:1], turned[HEAD_DIM:HEAD_DIM + 1]], axis=0)
        for copy in part_copies(k, slot, p, target):
            copy.start()

    def join(p, slots):
        outs, sums = [held_o[p]], [held_l[p]]
        for slot in slots:
            for copy in part_copies(0, slot, p, 0):
                copy.wait_recv()
            outs.append(got_o[slot, p].astype(jnp.float32))
            lse = got_l[slot, p]
            sums.append(jnp.transpose(jnp.concatenate(
                [jnp.broadcast_to(lse[h:h + 1], (HEAD_DIM, 2 * L)) for h in range(2)], axis=0)))
        peak = functools.reduce(jnp.maximum, sums)
        scale = [jnp.exp(s - peak) for s in sums]
        finish(p, sum(o * s for o, s in zip(outs, scale)) / sum(scale))

    def each(body, begin=0, end=None):
        def step(p, carry):
            body(p)
            return carry
        lax.fori_loop(begin, pairs if end is None else end, step, 0)

    def gates_here():
        g_own.wait()
        g_copy.wait_recv()

    def gates_up(target):
        return remote(gb.at[pl.ds(0, 2)], gb.at[pl.ds(0, 2)], g_send.at[1], g_recv.at[2], sp=target * 2 + x)

    half = pairs // 2

    @pl.when(z == 0)
    def _():
        gates_here()
        gates_up(1).start()
        def push(p):
            arrived(p)
            to_z(kx.at[p], kz.at[p], 0, 0, p, 1).start()
            to_z(vx.at[p], vz.at[p], 1, 1, p, 1).start()
        each(push)
        def work(p):
            finish(p, attend_rows(qx[p], [(kx[p], vx[p], gates_of(0, p))], True)[0])
        each(work)
        pass_on(0, lent)
        def left(p):
            to_z(kx.at[p], kz.at[p], 0, 0, p, 1).wait_send()
            to_z(vx.at[p], vz.at[p], 1, 1, p, 1).wait_send()
        each(left)
        gates_up(1).wait_send()

    @pl.when(z == 1)
    def _():
        gates_here()
        gates_up(0).wait_recv()
        def work(p):
            arrived(p)
            to_z(kx.at[p], kz.at[p], 0, 0, p, 0).wait_recv()
            to_z(vx.at[p], vz.at[p], 1, 1, p, 0).wait_recv()
            lower = (kz[p], vz[p], gates_of(0, p))
            own = (kx[p], vx[p], gates_of(1, p))
            finish(p, attend_rows(qx[p], [lower, own], True)[0])
            for k in range(2):
                to_z(qx.at[p], qz.at[k, p], 0, 2 + k, p, 0).wait_recv()
                share(p, k, 0, 2 + k, *attend_rows(qz[k, p], [lower, own], False))
        each(work, 0, half)
        pass_on(0, lent)
        each(work, half)
        def left(p):
            for k in range(2):
                for copy in part_copies(k, 0, p, 2 + k):
                    copy.wait_send()
        each(left)

    @pl.when(z == 2)
    def _():
        def push(p):
            arrived(p)
            to_z(qx.at[p], qz.at[0, p], 0, 2, p, 1).start()
        each(push)
        gates_here()
        def work(p):
            own = (kx[p], vx[p], gates_of(2, p))
            held_o[p], held_l[p] = attend_rows(qx[p], [own], True)
            to_z(qx.at[p], qz.at[0, p], 0, 2, p, 1).wait_recv()
            share(p, 1, 1, 3, *attend_rows(qz[0, p], [own], False))
        each(work)
        pass_on(0, lent)
        each(lambda p: join(p, (0,)))
        def left(p):
            to_z(qx.at[p], qz.at[0, p], 0, 2, p, 1).wait_send()
            for copy in part_copies(1, 1, p, 3):
                copy.wait_send()
        each(left)

    @pl.when(z == 3)
    def _():
        def push(p):
            arrived(p)
            to_z(qx.at[p], qz.at[1, p], 0, 3, p, 1).start()
            to_z(qx.at[p], qz.at[0, p], 1, 2, p, 2).start()
        each(push)
        gates_here()
        def work(p):
            held_o[p], held_l[p] = attend_rows(qx[p], [(kx[p], vx[p], gates_of(3, p))], True)
        each(work)
        pass_on(0, lent)
        each(lambda p: join(p, (0, 1)))
        def left(p):
            to_z(qx.at[p], qz.at[1, p], 0, 3, p, 1).wait_send()
            to_z(qx.at[p], qz.at[0, p], 1, 2, p, 2).wait_send()
        each(left)

    pass_on(lent, W_CHUNKS)

    def whole(p):
        o_own(p).wait()
        o_copy(p).wait_recv()
    each(whole)

    def columns(r):
        return pl.ds(pl.multiple_of(r * w_cols, LANES), w_cols)

    w_own.wait()
    o_ref[:, columns(me_dp)] = jnp.dot(
        att[...], wall[me_dp], preferred_element_type=jnp.float32).astype(o_ref.dtype)
    p_copy.wait_recv()
    o_ref[:, columns(partner)] = jnp.dot(
        att[...], wall[partner], preferred_element_type=jnp.float32).astype(o_ref.dtype)
    crossed = (1 - row_y) * 2 + 1 - core
    order = list(range(lent)) + list(range(direct, W_CHUNKS)) + list(range(lent, direct))
    for at, s in enumerate(order):
        left = att[:, chunk(s)]
        for which, r in ((0, across), (1, crossed)):
            if which:
                forward(s).wait_recv()
            part = jnp.dot(left, wall[r, chunk(s)], preferred_element_type=jnp.float32)
            if at > 0:
                part = acc[which] + part
            if at < W_CHUNKS - 1:
                acc[which] = part
            else:
                o_ref[:, columns(r)] = part.astype(o_ref.dtype)

    p_copy.wait_send()
    g_copy.wait_send()
    def sent(p):
        o_copy(p).wait_send()
        for a in range(3):
            x_copy(a, p).wait_send()
    each(sent)
    for s in range(W_CHUNKS):
        if s < direct:
            y_copy(s).wait_send()
        if s < lent:
            lend(s).wait_send()
        forward(s).wait_send()


def fused(n, ndp, queries, keys, values, gate_totals, w_out):
    L, model = queries.shape[1], queries.shape[2]
    heads = gate_totals.shape[2] // 2
    pairs = heads * HEAD_DIM // LANES
    gates = jnp.transpose(gate_totals[0]).reshape(2, pairs, 2, L)
    w_rows, w_cols = w_out.shape
    bf16, f32 = jnp.bfloat16, jnp.float32
    dma = pltpu.SemaphoreType.DMA
    block = (pairs, 2 * L, LANES)
    out = pl.pallas_call(
        functools.partial(kernel, n, ndp),
        out_shape=jax.ShapeDtypeStruct((L, w_cols * ndp), bf16),
        in_specs=[pl.BlockSpec(memory_space=pl.ANY)] * 5,
        out_specs=pl.BlockSpec(memory_space=pltpu.VMEM),
        scratch_shapes=[
            *[pltpu.VMEM(block, bf16)] * 5,
            pltpu.VMEM((2,) + block, bf16),
            pltpu.VMEM((n, pairs, 2, L), f32),
            pltpu.VMEM(block, bf16),
            pltpu.VMEM(block, f32),
            pltpu.VMEM(block, f32),
            pltpu.VMEM((2,) + block, bf16),
            pltpu.VMEM((2, pairs, 2, 2 * L), f32),
            pltpu.VMEM((2,) + block, bf16),
            pltpu.VMEM((2, pairs, 2, 2 * L), f32),
            pltpu.VMEM((L, model), bf16),
            pltpu.VMEM((ndp, w_rows, w_cols), bf16),
            pltpu.VMEM((2, L, w_cols), f32),
            dma((3, pairs)), dma((3, pairs)), dma((2,)), dma((3,)), dma((4, pairs + 1)),
            dma((2, pairs)), dma((4, pairs)),
            dma((2, pairs)), dma((2, pairs)), dma((2, pairs)), dma((2, pairs)),
            dma((pairs,)), dma((pairs,)),
            dma((W_CHUNKS,)), dma((W_CHUNKS,)), dma((W_CHUNKS,)), dma((W_CHUNKS,)), dma, dma,
            dma((W_CHUNKS,)), dma((W_CHUNKS,)),
        ],
        compiler_params=pltpu.CompilerParams(
            collective_id=0, has_side_effects=True, vmem_limit_bytes=67043328),
        name="fused_attention",
    )(queries[0], keys[0], values[0], gates, w_out)
    return out[None]


def solution(mesh):
    n, ndp = mesh.shape["sp"], mesh.shape["dp"]

    def local(queries, keys, values, gate_totals, w_out):
        fits = n == 8 and ndp == 4 and queries.shape[1] % LANES == 0
        if fits:
            return fused(n, ndp, queries, keys, values, gate_totals, w_out)
        return general(queries, keys, values, gate_totals, w_out)

    placed = (P("dp", "sp", None),) * 4 + (P(None, "dp"),)
    return jax.shard_map(
        local, mesh=mesh, in_specs=placed, out_specs=P("dp", "sp", None), check_vma=False)
```

```python
import functools

import jax
import jax.numpy as jnp
from jax import lax
from jax.experimental import pallas as pl
from jax.experimental.pallas import tpu as pltpu
from jax.sharding import PartitionSpec as P

HEAD_DIM = 64
LANES = 128
W_CHUNKS = 16
MESH = pl.DeviceIdType.MESH


def attend(queries, key_rows, value_rows, totals):
    length = queries.shape[0]
    block_rows = min(length, 512)
    pieces = []
    for begin_row in range(0, length, block_rows):
        end_row = begin_row + block_rows
        scaled = queries[begin_row:end_row] * jnp.bfloat16(HEAD_DIM ** (-0.5))
        scores = jnp.einsum(
            "qhd,khd->hqk", scaled, key_rows[:end_row], preferred_element_type=jnp.float32
        )
        causal = jnp.arange(end_row)[None, :] <= (begin_row + jnp.arange(block_rows))[:, None]
        scores = jnp.where(
            causal[None],
            scores
            + jnp.transpose(totals[begin_row:end_row])[:, :, None]
            - jnp.transpose(totals[:end_row])[:, None, :],
            -jnp.inf,
        )
        biggest = jnp.max(scores, axis=-1, keepdims=True)
        expo = jnp.exp(scores - biggest)
        summed = jnp.sum(expo, axis=-1)
        weights = expo.astype(jnp.bfloat16)
        output = jnp.einsum(
            "hqk,khd->qhd", weights, value_rows[:end_row], preferred_element_type=jnp.float32
        )
        output = output / jnp.transpose(summed)[:, :, None]
        pieces.append(output.astype(jnp.bfloat16))
    return jnp.concatenate(pieces, axis=0).reshape(length, -1)


def general(queries, keys, values, gate_totals, w_out):
    moved = [
        lax.all_to_all(x, "sp", split_axis=2, concat_axis=1, tiled=True)
        for x in (queries, keys, values, gate_totals)
    ]
    length = moved[0].shape[1]
    heads = [x[0].reshape(length, -1, HEAD_DIM) for x in moved[:3]]
    attended = attend(heads[0], heads[1], heads[2], moved[3][0])[None]
    rows = lax.all_to_all(attended, "sp", split_axis=1, concat_axis=2, tiled=True)
    mixed = jnp.dot(
        rows[0],
        lax.all_gather(w_out, "dp", axis=1, tiled=True),
        preferred_element_type=jnp.float32,
    )
    return mixed.astype(jnp.bfloat16)[None]


def attend_rows(queries, parts, diagonal):
    rows = queries.shape[0]
    scaled = queries * jnp.bfloat16(HEAD_DIM ** -0.5)
    lane = lax.broadcasted_iota(jnp.int32, (rows, LANES), 1)
    outs, sums = [], []
    for h in range(2):
        mine = (lane < HEAD_DIM) if h == 0 else (lane >= HEAD_DIM)
        scores = []
        for at, (keys, _, gates) in enumerate(parts):
            head_keys = jnp.where(mine, keys, jnp.zeros_like(keys))
            score = lax.dot_general(
                scaled, head_keys, (((1,), (1,)), ((), ())), preferred_element_type=jnp.float32)
            score = score - gates[h:h + 1, :]
            if diagonal and at == len(parts) - 1:
                causal = lax.broadcasted_iota(jnp.int32, score.shape, 1) <= lax.broadcasted_iota(
                    jnp.int32, score.shape, 0)
                score = jnp.where(causal, score, -jnp.inf)
            scores.append(score)
        peak = functools.reduce(jnp.maximum, [jnp.max(x, axis=1, keepdims=True) for x in scores])
        expo = [jnp.exp(x - peak) for x in scores]
        total = sum(jnp.sum(x, axis=1, keepdims=True) for x in expo)
        out = sum(
            jnp.dot(x.astype(jnp.bfloat16), part[1], preferred_element_type=jnp.float32)
            for x, part in zip(expo, parts))
        outs.append(out / total)
        sums.append(peak + jnp.log(total))
    first = lane < HEAD_DIM
    return jnp.where(first, outs[0], outs[1]), jnp.where(first, sums[0], sums[1])


def kernel(n, ndp, q_ref, k_ref, v_ref, g_ref, w_ref, o_ref,
           qx, kx, vx, kz, vz, qz, gb, ob, held_o, held_l, part_o, part_l, got_o, got_l, att, wall, acc,
           x_send, x_recv, g_send, g_recv, own_sem, z_send, z_recv, po_send, po_recv, pl_send, pl_recv,
           o_send, o_recv, y_send, y_recv, wx_send, wx_recv, p_send, p_recv, f_send, f_recv):
    me = lax.axis_index("sp")
    x = lax.rem(me, 2)
    z = lax.div(me, 2)
    side = me + 1 - 2 * x
    me_dp = lax.axis_index("dp")
    core = lax.rem(me_dp, 2)
    row_y = lax.div(me_dp, 2)
    across = (1 - row_y) * 2 + core
    partner = row_y * 2 + 1 - core
    L = q_ref.shape[0]
    pairs = qx.shape[0]
    W = pairs * LANES
    w_rows, w_cols = w_ref.shape
    step_rows = w_rows // W_CHUNKS
    lent = W_CHUNKS // 8
    direct = W_CHUNKS - lent

    barrier = pltpu.get_barrier_semaphore()
    meets = {0: (1,), 1: (0, 2, 3), 2: (1, 3), 3: (1, 2)}
    for here, others in meets.items():
        @pl.when(z == here)
        def _(others=others):
            for other in others:
                pl.semaphore_signal(barrier, inc=1, device_id={"sp": other * 2 + x}, device_id_type=MESH)
    pl.semaphore_signal(barrier, inc=1, device_id={"sp": side}, device_id_type=MESH)
    for other in (partner, across):
        pl.semaphore_signal(barrier, inc=1, device_id={"dp": other}, device_id_type=MESH)
    for here, others in meets.items():
        @pl.when(z == here)
        def _(others=others):
            pl.semaphore_wait(barrier, len(others) + 3)

    def remote(src, dst, send, recv, **device):
        return pltpu.make_async_remote_copy(
            src_ref=src, dst_ref=dst, send_sem=send, recv_sem=recv, device_id=device, device_id_type=MESH)

    def rows_of(which):
        return pl.ds(pl.multiple_of(which * L, L), L)

    def lanes_of(which, p):
        return pl.ds(pl.multiple_of(which * W + p * LANES, LANES), LANES)

    bufs = ((q_ref, qx), (k_ref, kx), (v_ref, vx))

    def x_copy(a, p):
        src, dst = bufs[a]
        return remote(src.at[:, lanes_of(1 - x, p)], dst.at[p, rows_of(x), :],
                      x_send.at[a, p], x_recv.at[a, p], sp=side)

    def x_own(a, p):
        src, dst = bufs[a]
        return pltpu.make_async_copy(src.at[:, lanes_of(x, p)], dst.at[p, rows_of(x), :], own_sem.at[a, p])

    g_copy = remote(g_ref.at[1 - x], gb.at[me], g_send.at[0], g_recv.at[0], sp=side)
    g_own = pltpu.make_async_copy(g_ref.at[x], gb.at[me], g_recv.at[1])

    def chunk(s):
        if s < lent:
            at = s + direct * x
        elif s < direct:
            at = s
        else:
            at = (s - direct) + direct * (1 - x)
        return pl.ds(pl.multiple_of(at * step_rows, step_rows), step_rows)

    def y_copy(s):
        return remote(w_ref.at[chunk(s)], wall.at[me_dp, chunk(s)], y_send.at[s], y_recv.at[s], dp=across)

    def lend(s):
        return remote(wall.at[across, chunk(s)], wall.at[across, chunk(s)], wx_send.at[s], wx_recv.at[s], sp=side)

    def forward(s):
        return remote(wall.at[across, chunk(s)], wall.at[across, chunk(s)], f_send.at[s], f_recv.at[s], dp=partner)

    p_copy = remote(w_ref, wall.at[me_dp], p_send, p_recv, dp=partner)
    w_own = pltpu.make_async_copy(w_ref, wall.at[me_dp], own_sem.at[3, 0])

    for p in range(pairs):
        for a in range(3):
            x_copy(a, p).start()
        if p == 0:
            g_copy.start()
            for s in range(direct):
                y_copy(s).start()
            g_own.start()
        for a in range(3):
            x_own(a, p).start()
    p_copy.start()
    w_own.start()

    def pass_on(begin, end):
        for s in range(begin, end):
            if s < direct:
                y_copy(s).wait_recv()
            else:
                lend(s - direct).wait_recv()
            forward(s).start()
            if s < lent:
                lend(s).start()

    def arrived(p):
        for a in range(3):
            x_own(a, p).wait()
            x_copy(a, p).wait_recv()

    def to_z(src, dst, k, slot, p, target):
        return remote(src, dst, z_send.at[k, p], z_recv.at[slot, p], sp=target * 2 + x)

    def part_copies(k, slot, p, target):
        return (
            remote(part_o.at[k, p], got_o.at[slot, p], po_send.at[k, p], po_recv.at[slot, p], sp=target * 2 + x),
            remote(part_l.at[k, p], got_l.at[slot, p], pl_send.at[k, p], pl_recv.at[slot, p], sp=target * 2 + x),
        )

    def o_copy(p):
        return remote(ob.at[p, rows_of(1 - x), :], att.at[:, lanes_of(x, p)], o_send.at[p], o_recv.at[p], sp=side)

    def o_own(p):
        return pltpu.make_async_copy(ob.at[p, rows_of(x), :], att.at[:, lanes_of(x, p)], own_sem.at[3, 1 + p])

    def gates_of(block, p):
        return jnp.concatenate([gb[2 * block, p], gb[2 * block + 1, p]], axis=1)

    def finish(p, value):
        ob[p] = value.astype(jnp.bfloat16)
        o_copy(p).start()
        o_own(p).start()

    def share(p, k, slot, target, value, lse):
        part_o[k, p] = value.astype(jnp.bfloat16)
        turned = jnp.transpose(lse)
        part_l[k, p] = jnp.concatenate([turned[0:1], turned[HEAD_DIM:HEAD_DIM + 1]], axis=0)
        for copy in part_copies(k, slot, p, target):
            copy.start()

    def join(p, slots):
        outs, sums = [held_o[p]], [held_l[p]]
        for slot in slots:
            for copy in part_copies(0, slot, p, 0):
                copy.wait_recv()
            outs.append(got_o[slot, p].astype(jnp.float32))
            lse = got_l[slot, p]
            sums.append(jnp.transpose(jnp.concatenate(
                [jnp.broadcast_to(lse[h:h + 1], (HEAD_DIM, 2 * L)) for h in range(2)], axis=0)))
        peak = functools.reduce(jnp.maximum, sums)
        scale = [jnp.exp(s - peak) for s in sums]
        finish(p, sum(o * s for o, s in zip(outs, scale)) / sum(scale))

    def each(body, begin=0, end=None):
        def step(p, carry):
            body(p)
            return carry
        lax.fori_loop(begin, pairs if end is None else end, step, 0)

    def gates_here():
        g_own.wait()
        g_copy.wait_recv()

    def gates_up(target):
        return remote(gb.at[pl.ds(0, 2)], gb.at[pl.ds(0, 2)], g_send.at[1], g_recv.at[2], sp=target * 2 + x)

    half = pairs // 2

    @pl.when(z == 0)
    def _():
        gates_here()
        gates_up(1).start()
        def push(p):
            arrived(p)
            to_z(kx.at[p], kz.at[p], 0, 0, p, 1).start()
            to_z(vx.at[p], vz.at[p], 1, 1, p, 1).start()
        each(push)
        def work(p):
            finish(p, attend_rows(qx[p], [(kx[p], vx[p], gates_of(0, p))], True)[0])
        each(work)
        pass_on(0, lent)
        def left(p):
            to_z(kx.at[p], kz.at[p], 0, 0, p, 1).wait_send()
            to_z(vx.at[p], vz.at[p], 1, 1, p, 1).wait_send()
        each(left)
        gates_up(1).wait_send()

    @pl.when(z == 1)
    def _():
        gates_here()
        gates_up(0).wait_recv()
        def work(p):
            arrived(p)
            to_z(kx.at[p], kz.at[p], 0, 0, p, 0).wait_recv()
            to_z(vx.at[p], vz.at[p], 1, 1, p, 0).wait_recv()
            lower = (kz[p], vz[p], gates_of(0, p))
            own = (kx[p], vx[p], gates_of(1, p))
            finish(p, attend_rows(qx[p], [lower, own], True)[0])
            for k in range(2):
                to_z(qx.at[p], qz.at[k, p], 0, 2 + k, p, 0).wait_recv()
                share(p, k, 0, 2 + k, *attend_rows(qz[k, p], [lower, own], False))
        each(work, 0, half)
        pass_on(0, lent)
        each(work, half)
        def left(p):
            for k in range(2):
                for copy in part_copies(k, 0, p, 2 + k):
                    copy.wait_send()
        each(left)

    @pl.when(z == 2)
    def _():
        def push(p):
            arrived(p)
            to_z(qx.at[p], qz.at[0, p], 0, 2, p, 1).start()
        each(push)
        gates_here()
        def work(p):
            own = (kx[p], vx[p], gates_of(2, p))
            held_o[p], held_l[p] = attend_rows(qx[p], [own], True)
            to_z(qx.at[p], qz.at[0, p], 0, 2, p, 1).wait_recv()
            share(p, 1, 1, 3, *attend_rows(qz[0, p], [own], False))
        each(work)
        pass_on(0, lent)
        each(lambda p: join(p, (0,)))
        def left(p):
            to_z(qx.at[p], qz.at[0, p], 0, 2, p, 1).wait_send()
            for copy in part_copies(1, 1, p, 3):
                copy.wait_send()
        each(left)

    @pl.when(z == 3)
    def _():
        def push(p):
            arrived(p)
            to_z(qx.at[p], qz.at[1, p], 0, 3, p, 1).start()
            to_z(qx.at[p], qz.at[0, p], 1, 2, p, 2).start()
        each(push)
        gates_here()
        def work(p):
            held_o[p], held_l[p] = attend_rows(qx[p], [(kx[p], vx[p], gates_of(3, p))], True)
        each(work)
        pass_on(0, lent)
        each(lambda p: join(p, (0, 1)))
        def left(p):
            to_z(qx.at[p], qz.at[1, p], 0, 3, p, 1).wait_send()
            to_z(qx.at[p], qz.at[0, p], 1, 2, p, 2).wait_send()
        each(left)

    pass_on(lent, W_CHUNKS)

    def whole(p):
        o_own(p).wait()
        o_copy(p).wait_recv()
    each(whole)

    def columns(r):
        return pl.ds(pl.multiple_of(r * w_cols, LANES), w_cols)

    w_own.wait()
    o_ref[:, columns(me_dp)] = jnp.dot(
        att[...], wall[me_dp], preferred_element_type=jnp.float32).astype(o_ref.dtype)
    p_copy.wait_recv()
    o_ref[:, columns(partner)] = jnp.dot(
        att[...], wall[partner], preferred_element_type=jnp.float32).astype(o_ref.dtype)
    crossed = (1 - row_y) * 2 + 1 - core
    order = list(range(lent)) + list(range(direct, W_CHUNKS)) + list(range(lent, direct))
    for at, s in enumerate(order):
        left = att[:, chunk(s)]
        for which, r in ((0, across), (1, crossed)):
            if which:
                forward(s).wait_recv()
            part = jnp.dot(left, wall[r, chunk(s)], preferred_element_type=jnp.float32)
            if at > 0:
                part = acc[which] + part
            if at < W_CHUNKS - 1:
                acc[which] = part
            else:
                o_ref[:, columns(r)] = part.astype(o_ref.dtype)

    p_copy.wait_send()
    g_copy.wait_send()
    def sent(p):
        o_copy(p).wait_send()
        for a in range(3):
            x_copy(a, p).wait_send()
    each(sent)
    for s in range(W_CHUNKS):
        if s < direct:
            y_copy(s).wait_send()
        if s < lent:
            lend(s).wait_send()
        forward(s).wait_send()


def fused(n, ndp, queries, keys, values, gate_totals, w_out):
    L, model = queries.shape[1], queries.shape[2]
    heads = gate_totals.shape[2] // 2
    pairs = heads * HEAD_DIM // LANES
    gates = jnp.transpose(gate_totals[0]).reshape(2, pairs, 2, L)
    w_rows, w_cols = w_out.shape
    bf16, f32 = jnp.bfloat16, jnp.float32
    dma = pltpu.SemaphoreType.DMA
    block = (pairs, 2 * L, LANES)
    out = pl.pallas_call(
        functools.partial(kernel, n, ndp),
        out_shape=jax.ShapeDtypeStruct((L, w_cols * ndp), bf16),
        in_specs=[pl.BlockSpec(memory_space=pl.ANY)] * 5,
        out_specs=pl.BlockSpec(memory_space=pltpu.VMEM),
        scratch_shapes=[
            *[pltpu.VMEM(block, bf16)] * 5,
            pltpu.VMEM((2,) + block, bf16),
            pltpu.VMEM((n, pairs, 2, L), f32),
            pltpu.VMEM(block, bf16),
            pltpu.VMEM(block, f32),
            pltpu.VMEM(block, f32),
            pltpu.VMEM((2,) + block, bf16),
            pltpu.VMEM((2, pairs, 2, 2 * L), f32),
            pltpu.VMEM((2,) + block, bf16),
            pltpu.VMEM((2, pairs, 2, 2 * L), f32),
            pltpu.VMEM((L, model), bf16),
            pltpu.VMEM((ndp, w_rows, w_cols), bf16),
            pltpu.VMEM((2, L, w_cols), f32),
            dma((3, pairs)), dma((3, pairs)), dma((2,)), dma((3,)), dma((4, pairs + 1)),
            dma((2, pairs)), dma((4, pairs)),
            dma((2, pairs)), dma((2, pairs)), dma((2, pairs)), dma((2, pairs)),
            dma((pairs,)), dma((pairs,)),
            dma((W_CHUNKS,)), dma((W_CHUNKS,)), dma((W_CHUNKS,)), dma((W_CHUNKS,)), dma, dma,
            dma((W_CHUNKS,)), dma((W_CHUNKS,)),
        ],
        compiler_params=pltpu.CompilerParams(
            collective_id=0, has_side_effects=True, vmem_limit_bytes=67043328),
        name="fused_attention",
    )(queries[0], keys[0], values[0], gates, w_out)
    return out[None]


def solution(mesh):
    n, ndp = mesh.shape["sp"], mesh.shape["dp"]

    def local(queries, keys, values, gate_totals, w_out):
        fits = n == 8 and ndp == 4 and queries.shape[1] % LANES == 0
        if fits:
            return fused(n, ndp, queries, keys, values, gate_totals, w_out)
        return general(queries, keys, values, gate_totals, w_out)

    placed = (P("dp", "sp", None),) * 4 + (P(None, "dp"),)
    return jax.shard_map(
        local, mesh=mesh, in_specs=placed, out_specs=P("dp", "sp", None), check_vma=False)
```
